32 devices in a mesh: rep: 2 (over x), fs: 8 (over z, y), tp: 2 (over core).
Axes of the slice: x: 2, y: 2, z: 4, core: 2. Of those that a mesh axis runs over, the one named last changes fastest.
Arguments:
- tokens: bfloat16 [8192, 2048], P(('rep', 'fs'), 'tp'), may hold values from -6 to 6
- mix_gain: float32 [2048], replicated, may hold values from 0.1 to 1.9
- query_w: bfloat16 [2048, 2048], P('fs', 'tp'), may hold values from -0.125 to 0.125
- key_w: bfloat16 [2048, 2048], P('fs', 'tp'), may hold values from -0.125 to 0.125
- value_w: bfloat16 [2048, 4096], P('fs', 'tp'), may hold values from -0.125 to 0.125
- head_gain: float32 [8, 512], replicated, may hold values from 0.1 to 1.9
- out_w: bfloat16 [4096, 2048], P('tp', 'fs'), may hold values from -0.09375 to 0.09375
- chan_gain: float32 [2048], replicated, may hold values from 0.1 to 1.9
- up_w: bfloat16 [2048, 4096], P('fs', 'tp'), may hold values from -0.125 to 0.125
- down_w: bfloat16 [4096, 2048], P('tp', 'fs'), may hold values from -0.09375 to 0.09375
Outputs:
- layer_out: bfloat16 [8192, 2048], P(('rep', 'fs'), 'tp')
The draws below stay inside these ranges and needn't reach their ends.
All inputs are finite; a program needn't handle non-finite values.
Results may differ from the reference program's by a relative error of at most 0.019.
Values may be sent and summed in bfloat16 or wider, within the bound.
A program may use at most 128 MiB of HBM per device.

```python
import jax
import jax.numpy as jnp
from jax import lax

D = 2048
HEADS = 8
DK = 256
DV = 512
FF = 4096
BLOCK = 128
TOK = 512
TOKENS = 8192
N_TP = 2


def block_scale(key, dims, shards, low, high):
    def one(dim, blocks):
        draws = jax.random.uniform(jax.random.fold_in(jax.random.fold_in(key, 6), dim), (blocks,), jnp.float32, low / len(shards), high / len(shards))
        return jnp.repeat(jnp.exp(draws), dims[dim] // blocks).reshape((-1,) + (1,) * (len(dims) - dim - 1))

    level = one(*shards[0])
    for cut in shards[1:]:
        level = level * one(*cut)
    return level


def noise(stream_key, shape, deviation, bound, shards=(), kind=jnp.bfloat16):
    values = jax.random.normal(stream_key, shape, jnp.float32) * deviation
    if len(shards) > 0:
        values = block_scale(stream_key, shape, shards, -0.22, 0.18) * values
    return jnp.clip(values, min=-bound, max=bound).astype(kind)


def setup_inputs(seed: int = 0) -> dict:
    splits = jax.random.split(jax.random.key(seed), 11)
    return {
        "tokens": noise(splits[0], (TOKENS, D), 1.0, 6.0, ((0, 16), (1, 2))),
        "mix_gain": jnp.clip(1.0 + 0.18 * jax.random.normal(splits[1], (D,), jnp.float32), 0.1, 1.9),
        "query_w": noise(splits[2], (D, D), D ** -0.5, 0.125, ((0, 8), (1, 2))),
        "key_w": noise(splits[3], (D, D), D ** -0.5, 0.125, ((0, 8), (1, 2))),
        "value_w": noise(splits[4], (D, HEADS * DV), D ** -0.5, 0.125, ((0, 8), (1, 2))),
        "head_gain": jnp.clip(1.0 + 0.18 * jax.random.normal(splits[5], (HEADS, DV), jnp.float32), 0.1, 1.9),
        "out_w": noise(splits[6], (HEADS * DV, D), (HEADS * DV) ** -0.5, 0.09375, ((0, 2), (1, 8))),
        "chan_gain": jnp.clip(1.0 + 0.18 * jax.random.normal(splits[7], (D,), jnp.float32), 0.1, 1.9),
        "up_w": noise(splits[8], (D, FF), D ** -0.5, 0.125, ((0, 8), (1, 2))),
        "down_w": noise(splits[9], (FF, D), FF ** -0.5, 0.09375, ((0, 2), (1, 8))),
    }


EPS = 1e-06
HEAD_EPS = 0.05
THETA = 10000.0

def norm_rows(rows, gain):
    values = rows.astype(jnp.float32)
    scale = lax.rsqrt(lax.optimization_barrier(jnp.mean(values * values, axis=-1, keepdims=True)) + EPS)
    return (values * scale * gain).astype(jnp.bfloat16)

def rotate(field, places):
    half = field.shape[-1] // 2
    inverse = THETA ** (-jnp.arange(half, dtype=jnp.float32) / half)
    angles = places[:, None] * inverse
    cosine = jnp.cos(angles)[:, None, :]
    sine = jnp.sin(angles)[:, None, :]
    first = field[..., :half]
    second = field[..., half:]
    return jnp.concatenate([first * cosine - second * sine, second * cosine + first * sine], axis=-1)

def retain(query, keys, values, log_rate):
    count = query.shape[0] // BLOCK
    q_blocks = query.reshape(count, BLOCK, query.shape[1])
    k_blocks = keys.reshape(count, BLOCK, keys.shape[1])
    v_blocks = values.reshape(count, BLOCK, values.shape[1])
    place = jnp.arange(BLOCK, dtype=jnp.float32)
    offset = place[:, None] - place[None, :]
    mask = jnp.where(offset >= 0, jnp.exp(log_rate * jnp.maximum(offset, 0.0)), 0.0)
    q_decay = jnp.exp(log_rate * (place + 1.0))
    k_decay = jnp.exp(log_rate * (BLOCK - 1.0 - place))
    block_decay = jnp.exp(log_rate * BLOCK)

    def advance(state, item):
        q_part, k_part, v_part = item
        scores = jnp.dot(q_part, k_part.T, preferred_element_type=jnp.float32)
        weights = (scores * mask).astype(jnp.bfloat16)
        result = jnp.dot(weights, v_part, preferred_element_type=jnp.float32)
        q_scaled = (q_part.astype(jnp.float32) * q_decay[:, None]).astype(jnp.bfloat16)
        result = result + jnp.dot(q_scaled, state.astype(jnp.bfloat16), preferred_element_type=jnp.float32)
        k_scaled = (k_part.astype(jnp.float32) * k_decay[:, None]).astype(jnp.bfloat16)
        state = state * block_decay + jnp.dot(k_scaled.T, v_part, preferred_element_type=jnp.float32)
        return (state, result)
    start = jnp.zeros((query.shape[1], values.shape[1]), jnp.float32)
    _, outputs = lax.scan(advance, start, (q_blocks, k_blocks, v_blocks))
    return outputs.reshape(count * BLOCK, values.shape[1])

def grouped_sum(left, right):
    width = left.shape[1] // N_TP
    total = jnp.zeros((left.shape[0], right.shape[1]), jnp.float32)
    for group in range(N_TP):
        term = jnp.dot(left[:, group * width:(group + 1) * width], right[group * width:(group + 1) * width], preferred_element_type=jnp.float32).astype(jnp.bfloat16)
        term = lax.optimization_barrier(term)
        total = total + term.astype(jnp.float32)
    return total

def reference(tokens, mix_gain, query_w, key_w, value_w, head_gain, out_w, chan_gain, up_w, down_w):
    normed = norm_rows(tokens, mix_gain)
    qraw = jnp.dot(normed, query_w, preferred_element_type=jnp.float32)
    kraw = jnp.dot(normed, key_w, preferred_element_type=jnp.float32)
    vraw = jnp.dot(normed, value_w, preferred_element_type=jnp.float32)
    places = (jnp.arange(TOKENS, dtype=jnp.int32) % TOK).astype(jnp.float32)
    query = rotate(qraw.reshape(TOKENS, HEADS, DK), places).astype(jnp.bfloat16)
    keys = (rotate(kraw.reshape(TOKENS, HEADS, DK), places) * DK ** (-0.5)).astype(jnp.bfloat16)
    values = vraw.reshape(TOKENS, HEADS, DV).astype(jnp.bfloat16)
    heads = jnp.arange(HEADS, dtype=jnp.int32).astype(jnp.float32)
    log_rate = jnp.log1p(-jnp.exp2(-5.0 - heads))
    count = TOKENS // TOK
    per_head = jax.vmap(retain, in_axes=(1, 1, 1, 0), out_axes=1)

    def one_sequence(item):
        return per_head(item[0], item[1], item[2], log_rate)
    retained = lax.map(one_sequence, (query.reshape(count, TOK, HEADS, DK), keys.reshape(count, TOK, HEADS, DK), values.reshape(count, TOK, HEADS, DV)))
    retained = retained.reshape(TOKENS, HEADS, DV)
    scale = lax.rsqrt(lax.optimization_barrier(jnp.mean(retained * retained, axis=-1, keepdims=True)) + HEAD_EPS)
    head_out = (retained * scale * head_gain).astype(jnp.bfloat16).reshape(TOKENS, HEADS * DV)
    middle = (tokens.astype(jnp.float32) + grouped_sum(head_out, out_w)).astype(jnp.bfloat16)
    chan_normed = norm_rows(middle, chan_gain)
    upward = jnp.dot(chan_normed, up_w, preferred_element_type=jnp.float32)
    hidden = jnp.square(jax.nn.relu(upward)).astype(jnp.bfloat16)
    return (middle.astype(jnp.float32) + grouped_sum(hidden, down_w)).astype(jnp.bfloat16)
```

```python
import jax
import jax.numpy as jnp
from jax import lax
from jax.sharding import PartitionSpec as P

DK = 256
DV = 512
BLOCK = 128


EPS = 1e-06
HEAD_EPS = 0.05
THETA = 10000.0


def norm_rows(rows, gain):
    values = rows.astype(jnp.float32)
    scale = lax.rsqrt(jnp.mean(values * values, axis=-1, keepdims=True) + EPS)
    return (values * scale * gain).astype(jnp.bfloat16)


def rotate(field, places):
    half = field.shape[-1] // 2
    inverse = THETA ** (-jnp.arange(half, dtype=jnp.float32) / half)
    angles = places[:, None] * inverse
    cosine = jnp.cos(angles)[:, None, :]
    sine = jnp.sin(angles)[:, None, :]
    first = field[..., :half]
    second = field[..., half:]
    return jnp.concatenate(
        [first * cosine - second * sine, second * cosine + first * sine], axis=-1
    )


def retain(query, keys, values, log_rate):
    count = query.shape[0] // BLOCK
    q_blocks = query.reshape(count, BLOCK, query.shape[1])
    k_blocks = keys.reshape(count, BLOCK, keys.shape[1])
    v_blocks = values.reshape(count, BLOCK, values.shape[1])
    place = jnp.arange(BLOCK, dtype=jnp.float32)
    offset = place[:, None] - place[None, :]
    mask = jnp.where(offset >= 0, jnp.exp(log_rate * jnp.maximum(offset, 0.0)), 0.0)
    q_decay = jnp.exp(log_rate * (place + 1.0))
    k_decay = jnp.exp(log_rate * (BLOCK - 1.0 - place))
    block_decay = jnp.exp(log_rate * BLOCK)

    def advance(state, item):
        q_part, k_part, v_part = item
        scores = jnp.dot(q_part, k_part.T, preferred_element_type=jnp.float32)
        weights = (scores * mask).astype(jnp.bfloat16)
        result = jnp.dot(weights, v_part, preferred_element_type=jnp.float32)
        q_scaled = (q_part.astype(jnp.float32) * q_decay[:, None]).astype(jnp.bfloat16)
        result = result + jnp.dot(
            q_scaled, state.astype(jnp.bfloat16), preferred_element_type=jnp.float32
        )
        k_scaled = (k_part.astype(jnp.float32) * k_decay[:, None]).astype(jnp.bfloat16)
        state = state * block_decay + jnp.dot(
            k_scaled.T, v_part, preferred_element_type=jnp.float32
        )
        return (state, result)

    start = jnp.zeros((query.shape[1], values.shape[1]), jnp.float32)
    _, outputs = lax.scan(advance, start, (q_blocks, k_blocks, v_blocks))
    return outputs.reshape(count * BLOCK, values.shape[1])


def shards(tokens, mix_gain, query_w, key_w, value_w, head_gain, out_w, chan_gain, up_w, down_w):
    rows = tokens.shape[0]
    local = query_w.shape[1] // DK
    whole = lax.all_gather(tokens, "tp", axis=1, tiled=True)
    normed = norm_rows(whole, mix_gain)
    pieces = (
        lax.all_gather(query_w, "fs", axis=0, tiled=True),
        lax.all_gather(key_w, "fs", axis=0, tiled=True),
        lax.all_gather(value_w, "fs", axis=0, tiled=True),
    )
    inputs = normed
    qraw, kraw, vraw = tuple(
        (jnp.dot(inputs, piece, preferred_element_type=jnp.float32) for piece in pieces)
    )
    places = jnp.arange(rows, dtype=jnp.int32).astype(jnp.float32)
    query = rotate(qraw.reshape(rows, local, DK), places).astype(jnp.bfloat16)
    keys = (rotate(kraw.reshape(rows, local, DK), places) * DK ** (-0.5)).astype(jnp.bfloat16)
    values = vraw.reshape(rows, local, DV).astype(jnp.bfloat16)
    first_head = lax.axis_index("tp") * local
    heads = (first_head + jnp.arange(local, dtype=jnp.int32)).astype(jnp.float32)
    log_rate = jnp.log1p(-jnp.exp2(-5.0 - heads))
    retained = jax.vmap(retain, in_axes=(1, 1, 1, 0), out_axes=1)(query, keys, values, log_rate)
    gains = lax.dynamic_slice_in_dim(head_gain, first_head, local, 0)
    scale = lax.rsqrt(jnp.mean(retained * retained, axis=-1, keepdims=True) + HEAD_EPS)
    head_out = (retained * scale * gains).astype(jnp.bfloat16).reshape(rows, local * DV)
    mixer_terms = jnp.dot(
        head_out,
        lax.all_gather(out_w, "fs", axis=1, tiled=True),
        preferred_element_type=jnp.float32,
    )
    mixed = lax.psum_scatter(
        mixer_terms.astype(jnp.bfloat16), "tp", scatter_dimension=1, tiled=True
    ).astype(jnp.float32)
    middle = (tokens.astype(jnp.float32) + mixed).astype(jnp.bfloat16)
    whole_middle = lax.all_gather(middle, "tp", axis=1, tiled=True)
    chan_normed = norm_rows(whole_middle, chan_gain)
    inputs = chan_normed
    upward = jnp.dot(
        inputs, lax.all_gather(up_w, "fs", axis=0, tiled=True), preferred_element_type=jnp.float32
    )
    hidden = jnp.square(jax.nn.relu(upward)).astype(jnp.bfloat16)
    chan_terms = jnp.dot(
        hidden, lax.all_gather(down_w, "fs", axis=1, tiled=True), preferred_element_type=jnp.float32
    )
    channel = lax.psum_scatter(
        chan_terms.astype(jnp.bfloat16), "tp", scatter_dimension=1, tiled=True
    ).astype(jnp.float32)
    return (middle.astype(jnp.float32) + channel).astype(jnp.bfloat16)


def half_of(block, axis, index, count):
    size = block.shape[axis] // count
    return lax.dynamic_slice_in_dim(block, index * size, size, axis)


def split_shards(
    parts, tps, tokens, mix_gain, query_w, key_w, value_w, head_gain, out_w, chan_gain, up_w, down_w
):
    rows, width = tokens.shape
    group = ("rep", "tp")
    rep = lax.axis_index("rep")

    def join(block):
        whole = lax.all_gather(block, group, axis=0, tiled=False)
        whole = whole.reshape(parts, tps, rows, width).transpose(0, 2, 1, 3)
        return whole.reshape(parts * rows, tps * width)

    def scatter(terms):
        pieces = terms.astype(jnp.bfloat16).reshape(parts, rows, tps, width).transpose(0, 2, 1, 3)
        pieces = pieces.reshape(parts * tps * rows, width)
        return lax.psum_scatter(pieces, group, scatter_dimension=0, tiled=True).astype(jnp.float32)

    local = query_w.shape[1] // DK // parts
    mine = jnp.concatenate(
        [half_of(w, 1, rep, parts) for w in (query_w, key_w, value_w)], axis=1
    )
    normed = norm_rows(join(tokens), mix_gain)
    raw = jnp.dot(
        normed,
        lax.all_gather(mine, "fs", axis=0, tiled=True),
        preferred_element_type=jnp.float32,
    )
    qraw, kraw, vraw = jnp.split(raw, [local * DK, 2 * local * DK], axis=1)
    places = jnp.arange(rows, dtype=jnp.int32).astype(jnp.float32)
    places = jnp.tile(places, parts)
    query = rotate(qraw.reshape(parts * rows, local, DK), places).astype(jnp.bfloat16)
    keys = (rotate(kraw.reshape(parts * rows, local, DK), places) * DK ** (-0.5)).astype(
        jnp.bfloat16
    )
    values = vraw.reshape(parts * rows, local, DV).astype(jnp.bfloat16)
    first_head = (lax.axis_index("tp") * parts + rep) * local
    heads = (first_head + jnp.arange(local, dtype=jnp.int32)).astype(jnp.float32)
    log_rate = jnp.log1p(-jnp.exp2(-5.0 - heads))
    over_heads = jax.vmap(retain, in_axes=(1, 1, 1, 0), out_axes=1)
    over_sequences = jax.vmap(over_heads, in_axes=(0, 0, 0, None), out_axes=0)
    retained = over_sequences(
        query.reshape(parts, rows, local, DK),
        keys.reshape(parts, rows, local, DK),
        values.reshape(parts, rows, local, DV),
        log_rate,
    ).reshape(parts * rows, local, DV)
    gains = lax.dynamic_slice_in_dim(head_gain, first_head, local, 0)
    scale = lax.rsqrt(jnp.mean(retained * retained, axis=-1, keepdims=True) + HEAD_EPS)
    head_out = (retained * scale * gains).astype(jnp.bfloat16).reshape(parts * rows, local * DV)
    out_all = lax.all_gather(half_of(out_w, 0, rep, parts), "fs", axis=1, tiled=True)
    mixed = scatter(jnp.dot(head_out, out_all, preferred_element_type=jnp.float32))
    middle = (tokens.astype(jnp.float32) + mixed).astype(jnp.bfloat16)
    chan_normed = norm_rows(join(middle), chan_gain)
    up_all = lax.all_gather(half_of(up_w, 1, rep, parts), "fs", axis=0, tiled=True)
    upward = jnp.dot(chan_normed, up_all, preferred_element_type=jnp.float32)
    hidden = jnp.square(jax.nn.relu(upward)).astype(jnp.bfloat16)
    down_all = lax.all_gather(half_of(down_w, 0, rep, parts), "fs", axis=1, tiled=True)
    channel = scatter(jnp.dot(hidden, down_all, preferred_element_type=jnp.float32))
    return (middle.astype(jnp.float32) + channel).astype(jnp.bfloat16)


def solution(mesh):
    placed = (
        P(("rep", "fs"), "tp"),
        P(),
        P("fs", "tp"),
        P("fs", "tp"),
        P("fs", "tp"),
        P(),
        P("tp", "fs"),
        P(),
        P("fs", "tp"),
        P("tp", "fs"),
    )
    parts, tps = mesh.shape["rep"], mesh.shape["tp"]

    def body(*blocks):
        if blocks[2].shape[1] // DK % parts == 0:
            return split_shards(parts, tps, *blocks)
        return shards(*blocks)

    return jax.shard_map(
        body, mesh=mesh, in_specs=placed, out_specs=P(("rep", "fs"), "tp"), check_vma=False
    )
```

```python
import functools

import jax
import jax.numpy as jnp
from jax import lax
from jax.experimental import pallas as pl
from jax.experimental.pallas import tpu as pltpu
from jax.sharding import PartitionSpec as P

DK = 256
DV = 512
BLOCK = 128


EPS = 1e-06
HEAD_EPS = 0.05
THETA = 10000.0


def norm_rows(rows, gain):
    values = rows.astype(jnp.float32)
    scale = lax.rsqrt(jnp.mean(values * values, axis=-1, keepdims=True) + EPS)
    return (values * scale * gain).astype(jnp.bfloat16)


def rotate(field, places):
    half = field.shape[-1] // 2
    inverse = THETA ** (-jnp.arange(half, dtype=jnp.float32) / half)
    angles = places[:, None] * inverse
    cosine = jnp.cos(angles)[:, None, :]
    sine = jnp.sin(angles)[:, None, :]
    first = field[..., :half]
    second = field[..., half:]
    return jnp.concatenate(
        [first * cosine - second * sine, second * cosine + first * sine], axis=-1
    )


def retain(query, keys, values, log_rate):
    count = query.shape[0] // BLOCK
    q_blocks = query.reshape(count, BLOCK, query.shape[1])
    k_blocks = keys.reshape(count, BLOCK, keys.shape[1])
    v_blocks = values.reshape(count, BLOCK, values.shape[1])
    place = jnp.arange(BLOCK, dtype=jnp.float32)
    offset = place[:, None] - place[None, :]
    mask = jnp.where(offset >= 0, jnp.exp(log_rate * jnp.maximum(offset, 0.0)), 0.0)
    q_decay = jnp.exp(log_rate * (place + 1.0))
    k_decay = jnp.exp(log_rate * (BLOCK - 1.0 - place))
    block_decay = jnp.exp(log_rate * BLOCK)

    def advance(state, item):
        q_part, k_part, v_part = item
        scores = jnp.dot(q_part, k_part.T, preferred_element_type=jnp.float32)
        weights = (scores * mask).astype(jnp.bfloat16)
        result = jnp.dot(weights, v_part, preferred_element_type=jnp.float32)
        q_scaled = (q_part.astype(jnp.float32) * q_decay[:, None]).astype(jnp.bfloat16)
        result = result + jnp.dot(
            q_scaled, state.astype(jnp.bfloat16), preferred_element_type=jnp.float32
        )
        k_scaled = (k_part.astype(jnp.float32) * k_decay[:, None]).astype(jnp.bfloat16)
        state = state * block_decay + jnp.dot(
            k_scaled.T, v_part, preferred_element_type=jnp.float32
        )
        return (state, result)

    start = jnp.zeros((query.shape[1], values.shape[1]), jnp.float32)
    _, outputs = lax.scan(advance, start, (q_blocks, k_blocks, v_blocks))
    return outputs.reshape(count * BLOCK, values.shape[1])


def shards(tokens, mix_gain, query_w, key_w, value_w, head_gain, out_w, chan_gain, up_w, down_w):
    rows = tokens.shape[0]
    local = query_w.shape[1] // DK
    whole = lax.all_gather(tokens, "tp", axis=1, tiled=True)
    normed = norm_rows(whole, mix_gain)
    pieces = (
        lax.all_gather(query_w, "fs", axis=0, tiled=True),
        lax.all_gather(key_w, "fs", axis=0, tiled=True),
        lax.all_gather(value_w, "fs", axis=0, tiled=True),
    )
    inputs = normed
    qraw, kraw, vraw = tuple(
        (jnp.dot(inputs, piece, preferred_element_type=jnp.float32) for piece in pieces)
    )
    places = jnp.arange(rows, dtype=jnp.int32).astype(jnp.float32)
    query = rotate(qraw.reshape(rows, local, DK), places).astype(jnp.bfloat16)
    keys = (rotate(kraw.reshape(rows, local, DK), places) * DK ** (-0.5)).astype(jnp.bfloat16)
    values = vraw.reshape(rows, local, DV).astype(jnp.bfloat16)
    first_head = lax.axis_index("tp") * local
    heads = (first_head + jnp.arange(local, dtype=jnp.int32)).astype(jnp.float32)
    log_rate = jnp.log1p(-jnp.exp2(-5.0 - heads))
    retained = jax.vmap(retain, in_axes=(1, 1, 1, 0), out_axes=1)(query, keys, values, log_rate)
    gains = lax.dynamic_slice_in_dim(head_gain, first_head, local, 0)
    scale = lax.rsqrt(jnp.mean(retained * retained, axis=-1, keepdims=True) + HEAD_EPS)
    head_out = (retained * scale * gains).astype(jnp.bfloat16).reshape(rows, local * DV)
    mixer_terms = jnp.dot(
        head_out,
        lax.all_gather(out_w, "fs", axis=1, tiled=True),
        preferred_element_type=jnp.float32,
    )
    mixed = lax.psum_scatter(
        mixer_terms.astype(jnp.bfloat16), "tp", scatter_dimension=1, tiled=True
    ).astype(jnp.float32)
    middle = (tokens.astype(jnp.float32) + mixed).astype(jnp.bfloat16)
    whole_middle = lax.all_gather(middle, "tp", axis=1, tiled=True)
    chan_normed = norm_rows(whole_middle, chan_gain)
    inputs = chan_normed
    upward = jnp.dot(
        inputs, lax.all_gather(up_w, "fs", axis=0, tiled=True), preferred_element_type=jnp.float32
    )
    hidden = jnp.square(jax.nn.relu(upward)).astype(jnp.bfloat16)
    chan_terms = jnp.dot(
        hidden, lax.all_gather(down_w, "fs", axis=1, tiled=True), preferred_element_type=jnp.float32
    )
    channel = lax.psum_scatter(
        chan_terms.astype(jnp.bfloat16), "tp", scatter_dimension=1, tiled=True
    ).astype(jnp.float32)
    return (middle.astype(jnp.float32) + channel).astype(jnp.bfloat16)


def ring_place(spot, count):
    turn = spot // (count // 2)
    return (1 - turn) * 2 * spot + turn * (2 * (count - 1 - spot) + 1)


def ring_kernel(count, axes, *refs):
    kinds = len(axes)
    sources, gathered = refs[:kinds], refs[kinds : 2 * kinds]
    send_sem, recv_sem, own_sem = refs[2 * kinds :]
    me = lax.axis_index("fs")
    column, level = me % 2, me // 2
    spot = (1 - column) * level + column * (count - 1 - level)
    ahead = ring_place((spot + 1) % count, count)
    behind = ring_place((spot + count - 1) % count, count)
    barrier = pltpu.get_barrier_semaphore()
    for other in (ahead, behind):
        pl.semaphore_signal(
            barrier, inc=1, device_id={"fs": other}, device_id_type=pl.DeviceIdType.MESH
        )
    pl.semaphore_wait(barrier, 2)
    steps = count // 2

    def slot(kind, origin):
        rows, columns = sources[kind].shape
        if axes[kind] == 0:
            return gathered[kind].at[pl.ds(pl.multiple_of(origin * rows, rows), rows), :]
        return gathered[kind].at[:, pl.ds(pl.multiple_of(origin * columns, columns), columns)]

    def piece(kind, origin, part):
        rows, columns = sources[kind].shape
        size = rows // 2
        if axes[kind] == 0:
            start = pl.multiple_of(origin * rows + part * size, size)
            return gathered[kind].at[pl.ds(start, size), :]
        start = pl.multiple_of(origin * columns, columns)
        return gathered[kind].at[pl.ds(part * size, size), pl.ds(start, columns)]

    def used(way, step, part):
        return step < steps - 1 or way == part

    def copy(kind, way, step, part):
        offset = count - step if way == 0 else step
        origin = ring_place((spot + offset) % count, count)
        target = piece(kind, origin, part)
        size = sources[kind].shape[0] // 2
        source = sources[kind].at[pl.ds(part * size, size), :] if step == 0 else target
        return pltpu.make_async_remote_copy(
            src_ref=source,
            dst_ref=target,
            send_sem=send_sem.at[kind, way, step, part],
            recv_sem=recv_sem.at[kind, way, step, part],
            device_id={"fs": ahead if way == 0 else behind},
            device_id_type=pl.DeviceIdType.MESH,
        )

    def own(kind):
        return pltpu.make_async_copy(sources[kind], slot(kind, me), own_sem.at[kind])

    for kind in range(kinds):
        own(kind).start()
        for step in range(steps):
            for part in range(2):
                for way in range(2):
                    if used(way, step, part):
                        if step > 0:
                            copy(kind, way, step - 1, part).wait_recv()
                        copy(kind, way, step, part).start()
    for kind in range(kinds):
        own(kind).wait()
        for step in range(steps):
            for part in range(2):
                for way in range(2):
                    if used(way, step, part):
                        copy(kind, way, step, part).wait_send()
                        last = step == steps - 1 or not used(way, step + 1, part)
                        if last:
                            copy(kind, way, step, part).wait_recv()


def ring_gather(count, axes, shards_in):
    shapes = []
    for axis, shard in zip(axes, shards_in):
        shape = list(shard.shape)
        shape[axis] *= count
        shapes.append(jax.ShapeDtypeStruct(tuple(shape), shard.dtype))
    kinds = len(axes)
    sems = (kinds, 2, count // 2, 2)
    return pl.pallas_call(
        functools.partial(ring_kernel, count, axes),
        out_shape=shapes,
        in_specs=[pl.BlockSpec(memory_space=pltpu.VMEM)] * kinds,
        out_specs=[pl.BlockSpec(memory_space=pl.ANY)] * kinds,
        scratch_shapes=[
            pltpu.SemaphoreType.DMA(sems),
            pltpu.SemaphoreType.DMA(sems),
            pltpu.SemaphoreType.DMA((kinds,)),
        ],
        compiler_params=pltpu.CompilerParams(collective_id=0, has_side_effects=True),
        cost_estimate=pl.CostEstimate(
            flops=40_000_000_000, bytes_accessed=60_000_000, transcendentals=0
        ),
        name="ring_gather",
    )(*shards_in)


def half_of(block, axis, index, count):
    size = block.shape[axis] // count
    return lax.dynamic_slice_in_dim(block, index * size, size, axis)


def split_shards(
    parts, tps, count, tokens, mix_gain, query_w, key_w, value_w, head_gain, out_w, chan_gain, up_w, down_w
):
    rows, width = tokens.shape
    group = ("rep", "tp")
    rep = lax.axis_index("rep")

    def join(block):
        whole = lax.all_gather(block, group, axis=0, tiled=False)
        whole = whole.reshape(parts, tps, rows, width).transpose(0, 2, 1, 3)
        return whole.reshape(parts * rows, tps * width)

    def scatter(terms):
        pieces = terms.astype(jnp.bfloat16).reshape(parts, rows, tps, width).transpose(0, 2, 1, 3)
        pieces = pieces.reshape(parts * tps * rows, width)
        return lax.psum_scatter(pieces, group, scatter_dimension=0, tiled=True).astype(jnp.float32)

    local = query_w.shape[1] // DK // parts
    mine = jnp.concatenate(
        [half_of(w, 1, rep, parts) for w in (query_w, key_w, value_w)], axis=1
    )
    out_half = half_of(out_w, 0, rep, parts)
    up_half = half_of(up_w, 1, rep, parts)
    down_half = half_of(down_w, 0, rep, parts)
    front_all, out_all, up_all, down_all = ring_gather(
        count, (0, 1, 0, 1), (mine, out_half, up_half, down_half)
    )
    normed = norm_rows(join(tokens), mix_gain)
    raw = jnp.dot(normed, front_all, preferred_element_type=jnp.float32)
    qraw, kraw, vraw = jnp.split(raw, [local * DK, 2 * local * DK], axis=1)
    places = jnp.arange(rows, dtype=jnp.int32).astype(jnp.float32)
    places = jnp.tile(places, parts)
    query = rotate(qraw.reshape(parts * rows, local, DK), places).astype(jnp.bfloat16)
    keys = (rotate(kraw.reshape(parts * rows, local, DK), places) * DK ** (-0.5)).astype(
        jnp.bfloat16
    )
    values = vraw.reshape(parts * rows, local, DV).astype(jnp.bfloat16)
    first_head = (lax.axis_index("tp") * parts + rep) * local
    heads = (first_head + jnp.arange(local, dtype=jnp.int32)).astype(jnp.float32)
    log_rate = jnp.log1p(-jnp.exp2(-5.0 - heads))
    over_heads = jax.vmap(retain, in_axes=(1, 1, 1, 0), out_axes=1)
    over_sequences = jax.vmap(over_heads, in_axes=(0, 0, 0, None), out_axes=0)
    retained = over_sequences(
        query.reshape(parts, rows, local, DK),
        keys.reshape(parts, rows, local, DK),
        values.reshape(parts, rows, local, DV),
        log_rate,
    ).reshape(parts * rows, local, DV)
    gains = lax.dynamic_slice_in_dim(head_gain, first_head, local, 0)
    scale = lax.rsqrt(jnp.mean(retained * retained, axis=-1, keepdims=True) + HEAD_EPS)
    head_out = (retained * scale * gains).astype(jnp.bfloat16).reshape(parts * rows, local * DV)
    mixed = scatter(jnp.dot(head_out, out_all, preferred_element_type=jnp.float32))
    middle = (tokens.astype(jnp.float32) + mixed).astype(jnp.bfloat16)
    chan_normed = norm_rows(join(middle), chan_gain)
    upward = jnp.dot(chan_normed, up_all, preferred_element_type=jnp.float32)
    hidden = jnp.square(jax.nn.relu(upward)).astype(jnp.bfloat16)
    channel = scatter(jnp.dot(hidden, down_all, preferred_element_type=jnp.float32))
    return (middle.astype(jnp.float32) + channel).astype(jnp.bfloat16)


def solution(mesh):
    placed = (
        P(("rep", "fs"), "tp"),
        P(),
        P("fs", "tp"),
        P("fs", "tp"),
        P("fs", "tp"),
        P(),
        P("tp", "fs"),
        P(),
        P("fs", "tp"),
        P("tp", "fs"),
    )
    parts, tps, count = mesh.shape["rep"], mesh.shape["tp"], mesh.shape["fs"]

    def body(*blocks):
        if blocks[2].shape[1] // DK % parts == 0 and count % 2 == 0:
            return split_shards(parts, tps, count, *blocks)
        return shards(*blocks)

    return jax.shard_map(
        body, mesh=mesh, in_specs=placed, out_specs=P(("rep", "fs"), "tp"), check_vma=False
    )
```
